32 devices in a mesh: grp: 2 (over y), fs: 4 (over z), tp: 4 (over x, core).
Axes of the slice: x: 2, y: 2, z: 4, core: 2. Of those that a mesh axis runs over, the one named last changes fastest.
Arguments:
- tokens: bfloat16 [4096, 2048], P(('grp', 'fs')), parts along dimension 0, may hold values from -6 to 6
- norm_in: bfloat16 [2048], replicated, may hold values from 0.099609375 to 1.8984375
- w_value: bfloat16 [2048, 2048], P('fs', 'tp'), may hold values from -0.125 to 0.125
- w_gate: bfloat16 [2048, 2048], P('fs', 'tp'), may hold values from -0.125 to 0.125
- conv_kernel: float32 [31, 2048], replicated, as said below
- ln_gain: bfloat16 [2048], replicated, may hold values from 0.099609375 to 1.8984375
- ln_shift: bfloat16 [2048], replicated, may hold values from -3 to 3
- w_out: bfloat16 [2048, 2048], P('tp', 'fs'), may hold values from -0.125 to 0.125
- norm_mlp: bfloat16 [2048], replicated, may hold values from 0.099609375 to 1.8984375
- w_up: bfloat16 [2048, 8192], P('fs', 'tp'), may hold values from -0.125 to 0.125
- w_down: bfloat16 [8192, 2048], P('tp', 'fs'), may hold values from -0.0625 to 0.0625
Outputs:
- layer_out: bfloat16 [4096, 2048], P(('grp', 'fs', 'tp')), parts along dimension 0
The draws below stay inside these ranges and needn't reach their ends.
There are 2 independent parts, one for each index of `grp`. The reference program is written for one: setup_inputs(seed, part) draws one part's arguments, and reference() takes and returns one part's arrays. A program takes and returns all parts, laid end to end along the dimension named above; an argument that names none is the same for every part. Nothing has to cross between parts.
Inputs may be any that keep to these rules, and one draw needn't show every extreme that they name: `conv_kernel`: a depthwise kernel.
All inputs are finite; a program needn't handle non-finite values.
Results may differ from the reference program's by a relative error of at most 0.018.
Values may be sent and summed in bfloat16 or wider, within the bound.
A program may use at most 64 MiB of HBM per device.

```python
import jax
import jax.numpy as jnp
from jax import lax

D = 2048
FF = 8192
KERNEL = 31
SEQ = 512
TOKENS = 2048
N_FS = 4
N_TP = 4


def draw_conv_kernel(key, part):
    first, second = jax.random.split(jax.random.fold_in(key, 11), 2)
    base = jnp.clip(jax.random.normal(first, (KERNEL, D), jnp.float32), -4.0, 4.0) / jnp.sqrt(jnp.float32(KERNEL))
    channel = jnp.arange(D, dtype=jnp.float32) / D
    rising = jnp.exp(jnp.log(3.0) * channel) * jax.random.uniform(second, (D,), jnp.float32, 0.6, 1.4)
    return (base * rising[None, :]).astype(jnp.float32)


def block_scale(key, shape, cuts, low, high):
    def one(position, blocks):
        draws = jax.random.uniform(jax.random.fold_in(jax.random.fold_in(key, 6), position), (blocks,), jnp.float32, low / len(cuts), high / len(cuts))
        return jnp.repeat(jnp.exp(draws), shape[position] // blocks).reshape((-1,) + (1,) * (len(shape) - position - 1))

    factor_of = one(*cuts[0])
    for cut in cuts[1:]:
        factor_of = factor_of * one(*cut)
    return factor_of


def normal_values(key, dims, spread, reach, shards=(), kind=jnp.bfloat16):
    result = spread * jax.random.normal(key, dims, jnp.float32)
    if shards:
        result = result * block_scale(key, dims, shards, -0.22, 0.18)
    return jnp.clip(result, -reach, reach).astype(kind)


def setup_inputs(seed: int = 0, part: int = 0) -> dict:
    seeds = jax.random.split(jax.random.key(seed), 12)
    part_keys = jax.random.split(jax.random.fold_in(seeds[11], part), 12)
    return {
        "tokens": normal_values(part_keys[0], (TOKENS, D), 1.0, 6.0, ((0, 4),)),
        "norm_in": jnp.clip(1.0 + 0.18 * jax.random.normal(seeds[1], (D,), jnp.float32), 0.099609375, 1.8984375).astype(jnp.bfloat16),
        "w_value": normal_values(seeds[2], (D, D), D ** -0.5, 0.125, ((0, 4), (1, 4))),
        "w_gate": normal_values(seeds[3], (D, D), D ** -0.5, 0.125, ((0, 4), (1, 4))),
        "conv_kernel": draw_conv_kernel(jax.random.fold_in(seeds[11], 71), part),
        "ln_gain": jnp.clip(1.0 + 0.18 * jax.random.normal(seeds[5], (D,), jnp.float32), 0.099609375, 1.8984375).astype(jnp.bfloat16),
        "ln_shift": normal_values(seeds[6], (D,), 0.5, 3.0),
        "w_out": normal_values(seeds[7], (D, D), D ** -0.5, 0.125, ((0, 4), (1, 4))),
        "norm_mlp": jnp.clip(1.0 + 0.18 * jax.random.normal(seeds[8], (D,), jnp.float32), 0.099609375, 1.8984375).astype(jnp.bfloat16),
        "w_up": normal_values(seeds[9], (D, FF), D ** -0.5, 0.125, ((0, 4), (1, 4))),
        "w_down": normal_values(seeds[10], (FF, D), FF ** -0.5, 0.0625, ((0, 4), (1, 4))),
    }


def rms_scale(values, gain):
    as_float = values.astype(jnp.float32)
    scaled = as_float * lax.rsqrt(lax.optimization_barrier(jnp.mean(as_float * as_float, axis=-1, keepdims=True)) + 1e-06)
    return scaled * gain.astype(jnp.float32)

def grouped_sum(left, right, groups):
    inner = left.shape[1] // groups
    partials = jnp.einsum('stc,tcd->std', left.reshape(left.shape[0], groups, inner).astype(jnp.float32), right.reshape(groups, inner, right.shape[1]).astype(jnp.float32), precision=lax.Precision.HIGHEST)
    rounded = lax.optimization_barrier(partials.astype(jnp.bfloat16))
    return lax.optimization_barrier(jnp.sum(rounded.astype(jnp.float32), axis=1))

def reference(tokens, norm_in, w_value, w_gate, conv_kernel, ln_gain, ln_shift, w_out, norm_mlp, w_up, w_down):

    def one_sequence(sequence):
        normed_in = rms_scale(sequence, norm_in).astype(jnp.bfloat16)
        values_f = jnp.dot(normed_in, w_value, preferred_element_type=jnp.float32)
        gate_act = jnp.dot(normed_in, w_gate, preferred_element_type=jnp.float32)
        gated = values_f * jax.nn.sigmoid(gate_act)
        padded = jnp.pad(gated, ((KERNEL - 1, 0), (0, 0)))
        convolved = jnp.zeros_like(gated)
        for tap_index in range(KERNEL):
            convolved = convolved + conv_kernel[tap_index][None, :] * padded[tap_index:tap_index + SEQ]
        chan_mean = lax.optimization_barrier(jnp.mean(convolved, axis=-1, keepdims=True))
        chan_msq = lax.optimization_barrier(jnp.mean(convolved * convolved, axis=-1, keepdims=True))
        variance = chan_msq - chan_mean * chan_mean
        normed = (convolved - chan_mean) * lax.rsqrt(variance + 1e-05)
        normed = normed * ln_gain.astype(jnp.float32) + ln_shift.astype(jnp.float32)
        activated = jax.nn.silu(normed).astype(jnp.bfloat16)
        mixed = grouped_sum(activated, w_out, N_TP)
        residual = sequence.astype(jnp.float32) + mixed
        normed_mlp = rms_scale(residual, norm_mlp).astype(jnp.bfloat16)
        up_act = jnp.dot(normed_mlp, w_up, preferred_element_type=jnp.float32)
        hidden = jnp.square(jax.nn.relu(up_act)).astype(jnp.bfloat16)
        return (residual + grouped_sum(hidden, w_down, N_TP)).astype(jnp.bfloat16)
    sequences = tokens.reshape(N_FS, SEQ, D)
    return lax.map(one_sequence, sequences).reshape(TOKENS, D)
```

```python
import functools

import jax
import jax.numpy as jnp
from jax import lax
from jax.experimental import pallas as pl
from jax.experimental.pallas import tpu as pltpu
from jax.sharding import PartitionSpec as P

MESH = pl.DeviceIdType.MESH
PIECES = 4
AHEAD = 3
PAD = 32


def rms_rows(x, gain):
    return x * lax.rsqrt(jnp.mean(x * x, axis=-1, keepdims=True) + 1e-06) * gain


def kernel(
    F, T,
    tok, norm_in, conv_k, ln_gain, ln_shift, norm_mlp, wv, wg, wo, wu, wd,
    out,
    normed, gv, gg, go, gu, gd, gated, conv, act, part, rs, resid, nm, hidden, fin, rs2,
    st_own, st_recv, nm_own,
    local_sem, zsend_r, zsend_l, zrecv_r, zrecv_l, ysend_r, ysend_l, yrecv_r, yrecv_l,
    st_send, st_rsem, rs_send, rs_rsem, ag_send, ag_rsem, fs_send, fs_rsem,
):
    g = lax.axis_index("grp")
    z = lax.axis_index("fs")
    t = lax.axis_index("tp")
    S, D = tok.shape
    R, C = wv.shape
    H = wu.shape[1]
    N = wo.shape[1]
    taps = conv_k.shape[0]
    rows = S // T
    R2, C2, H2 = R // 2, C // 2, H // 2
    HB, HC = H // PIECES, H2 // PIECES
    other = 1 - g
    n_chunks = 3 + 2 * PIECES
    first_down = 3 + PIECES

    def mult(i, k):
        return pl.multiple_of(i, k)

    def own(c, h):
        if c < 3:
            ref, size = ((wv, R2), (wg, R2), (wo, C2))[c]
            return ref.at[pl.ds(mult(h * size, size), size), :]
        if c < first_down:
            return wu.at[pl.ds(mult(h * R2, R2), R2), pl.ds((c - 3) * HB, HB)]
        return wd.at[pl.ds(mult(h * H2 + (c - first_down) * HC, HC), HC), :]

    def slot(c, src, h):
        if c < 2:
            return (gv, gg)[c].at[pl.ds(mult(src * R + h * R2, R2), R2), :]
        if c == 2:
            return go.at[src, pl.ds(mult(h * C2, C2), C2), :]
        if c < first_down:
            return gu.at[c - 3, pl.ds(mult(src * R + h * R2, R2), R2), :]
        return gd.at[src, pl.ds(mult(h * H2 + (c - first_down) * HC, HC), HC), :]

    def remote(src_ref, dst_ref, send, recv, device):
        return pltpu.make_async_remote_copy(
            src_ref=src_ref, dst_ref=dst_ref, send_sem=send, recv_sem=recv,
            device_id=device, device_id_type=MESH,
        )

    peers = [lax.rem(t + i, T) for i in range(T)]
    sources = [lax.rem(t - i + T, T) for i in range(T)]

    barrier = pltpu.get_barrier_semaphore()

    def greet(device):
        pl.semaphore_signal(barrier, inc=1, device_id=device, device_id_type=MESH)

    greet((other, z, t))
    for i in range(1, T):
        greet((g, z, peers[i]))

    @pl.when(z > 0)
    def _():
        greet((g, z - 1, t))

    @pl.when(z < F - 1)
    def _():
        greet((g, z + 1, t))

    ends = lax.div(z + F - 1, F) + lax.div(2 * F - 2 - z, F)
    pl.semaphore_wait(barrier, T + ends)

    ys, yr = (ysend_r, ysend_l), (yrecv_r, yrecv_l)

    def own_right(c):
        return remote(own(c, g), slot(c, z, g), zsend_r.at[c, 0], zrecv_r.at[c, 1], (g, z + 1, t))

    def own_left(c):
        return remote(own(c, g), slot(c, z, g), zsend_l.at[c, 0], zrecv_l.at[c, 1], (g, z - 1, t))

    def right_hop(c, d, src):
        return remote(slot(c, src, g), slot(c, src, g), zsend_r.at[c, d], zrecv_r.at[c, min(d + 1, F - 1)], (g, z + 1, t))

    def left_hop(c, d, src):
        return remote(slot(c, src, g), slot(c, src, g), zsend_l.at[c, d], zrecv_l.at[c, min(d + 1, F - 1)], (g, z - 1, t))

    def arrival(c, d, src, left):
        sems = zrecv_l if left else zrecv_r
        return remote(slot(c, src, g), slot(c, src, g), zsend_r.at[c, d], sems.at[c, d], (g, z, t))

    def across(c, d, src, left):
        return remote(slot(c, src, g), slot(c, src, g), ys[left].at[c, d], yr[left].at[c, d], (other, z, t))

    def across_arrival(c, d, src, left):
        return remote(slot(c, src, other), slot(c, src, other), ys[left].at[c, d], yr[left].at[c, d], (other, z, t))

    issued = [0]

    def own_upto(limit):
        while issued[0] < min(limit, n_chunks):
            c = issued[0]
            issued[0] += 1

            @pl.when(z < F - 1)
            def _():
                own_right(c).start()

            @pl.when(z > 0)
            def _():
                own_left(c).start()

    def both(d, body):
        @pl.when(z - d >= 0)
        def _():
            body(z - d, 0)

        @pl.when(z + d < F)
        def _():
            body(z + d, 1)

    def service(c, d):
        def body(src, left):
            arrival(c, d, src, left).wait_recv()
            if d < F - 1:
                if left:
                    @pl.when(z > 0)
                    def _():
                        left_hop(c, d, src).start()
                else:
                    @pl.when(z < F - 1)
                    def _():
                        right_hop(c, d, src).start()
            across(c, d, src, left).start()

        both(d, body)

    def service_all(c):
        own_upto(c + 1 + AHEAD)
        for d in range(1, F):
            service(c, d)

    def y_wait(c, d):
        both(d, lambda src, left: across_arrival(c, d, src, left).wait_recv())

    def y_wait_all(c):
        for d in range(1, F):
            y_wait(c, d)

    own_upto(1)
    copies = [
        pltpu.make_async_copy(wv, gv.at[pl.ds(mult(z * R, R), R), :], local_sem.at[0]),
        pltpu.make_async_copy(wg, gg.at[pl.ds(mult(z * R, R), R), :], local_sem.at[1]),
        pltpu.make_async_copy(wo, go.at[z], local_sem.at[2]),
        pltpu.make_async_copy(wd, gd.at[z], local_sem.at[3]),
    ]
    for j in range(PIECES):
        copies.append(
            pltpu.make_async_copy(
                wu.at[:, pl.ds(j * HB, HB)], gu.at[j, pl.ds(mult(z * R, R), R), :], local_sem.at[4 + j]
            )
        )
    for copy in copies:
        copy.start()
    own_upto(1 + AHEAD)

    block = 64

    def norm_step(i, carry):
        at = pl.ds(mult(i * block, block), block)
        x = tok[at, :].astype(jnp.float32)
        normed[at, :] = rms_rows(x, norm_in[...].astype(jnp.float32)).astype(jnp.bfloat16)
        return carry

    lax.fori_loop(0, S // block, norm_step, 0)
    for copy in copies:
        copy.wait()

    service_all(0)
    service_all(1)
    own_upto(3 + AHEAD)
    service(2, 1)
    y_wait_all(0)
    y_wait_all(1)

    tile = min(256, C)
    gated[0:PAD, :] = jnp.zeros((PAD, C), jnp.float32)

    def gate_step(i, carry):
        at = pl.ds(mult(i * tile, tile), tile)
        v = jnp.dot(normed[...], gv[:, at], preferred_element_type=jnp.float32)
        a = jnp.dot(normed[...], gg[:, at], preferred_element_type=jnp.float32)
        gated[PAD:, at] = v * jax.nn.sigmoid(a)
        return carry

    lax.fori_loop(0, C // tile, gate_step, 0)

    for d in range(2, F):
        service(2, d)

    span = 128
    lead = PAD - (taps - 1)

    def conv_step(i, carry):
        base = mult(i * span, span)
        first = jnp.zeros((span, 128), jnp.float32)
        second = jnp.zeros((span, 128), jnp.float32)
        for j in range(C // 128):
            lanes = pl.ds(j * 128, 128)
            window = gated[pl.ds(base, span + PAD), lanes]
            weights = conv_k[:, pl.ds(mult(t * C + j * 128, 128), 128)]
            acc = jnp.zeros((span, 128), jnp.float32)
            for k in range(taps):
                acc = acc + weights[k : k + 1, :] * window[lead + k : lead + k + span, :]
            conv[pl.ds(base, span), lanes] = acc
            first = first + acc
            second = second + acc * acc
        lane = lax.broadcasted_iota(jnp.int32, (span, 128), 1)
        both_sums = jnp.where(
            lane == 0,
            jnp.sum(first, axis=1, keepdims=True),
            jnp.where(lane == 1, jnp.sum(second, axis=1, keepdims=True), 0.0),
        )
        st_own[:, pl.ds(base, span)] = jnp.transpose(both_sums)[0:8, :]
        return carry

    lax.fori_loop(0, S // span, conv_step, 0)

    def stat_copy(i):
        return remote(st_own, st_recv.at[i], st_send.at[i], st_rsem.at[i], (g, z, peers[i]))

    for i in range(1, T):
        stat_copy(i).start()
    service_all(3)
    for i in range(1, T):
        stat_copy(i).wait_recv()

    gain = ln_gain[:, pl.ds(mult(t * C, C), C)].astype(jnp.float32)
    shift = ln_shift[:, pl.ds(mult(t * C, C), C)].astype(jnp.float32)

    def act_step(i, carry):
        base = mult(i * span, span)
        at = pl.ds(base, span)
        sums = st_own[:, at]
        for k in range(1, T):
            sums = sums + st_recv[k, :, at]
        mean = sums[0:1, :] / D
        var = sums[1:2, :] / D - mean * mean
        scale = lax.rsqrt(var + 1e-05)
        mean_c = jnp.transpose(jnp.broadcast_to(mean, (128, span)))[:, 0:1]
        scale_c = jnp.transpose(jnp.broadcast_to(scale, (128, span)))[:, 0:1]
        n = (conv[at, :] - mean_c) * scale_c * gain + shift
        act[at, :] = (n * jax.nn.sigmoid(n)).astype(jnp.bfloat16)
        return carry

    lax.fori_loop(0, S // span, act_step, 0)
    y_wait_all(2)

    def out_step(i, carry):
        part[:, pl.ds(mult(i * N, N), N)] = jnp.dot(
            act[...], go[i], preferred_element_type=jnp.float32
        ).astype(jnp.bfloat16)
        return carry

    lax.fori_loop(0, F, out_step, 0)

    def mix_copy(i):
        return remote(
            part.at[pl.ds(mult(peers[i] * rows, rows), rows), :], rs.at[i], rs_send.at[i], rs_rsem.at[i], (g, z, peers[i])
        )

    for i in range(1, T):
        mix_copy(i).start()
    service_all(4)
    service(5, 1)
    for i in range(1, T):
        mix_copy(i).wait_recv()

    small = 32

    def resid_step(i, carry):
        at = pl.ds(mult(i * small, small), small)
        mine = pl.ds(mult(t * rows + i * small, small), small)
        total = part[mine, :].astype(jnp.float32)
        for k in range(1, T):
            total = total + rs[k, at, :].astype(jnp.float32)
        r = tok[mine, :].astype(jnp.float32) + total
        resid[at, :] = r
        nm_own[at, :] = rms_rows(r, norm_mlp[...].astype(jnp.float32)).astype(jnp.bfloat16)
        return carry

    lax.fori_loop(0, rows // small, resid_step, 0)

    def norm_copy(i):
        return remote(
            nm_own, nm.at[pl.ds(mult(t * rows, rows), rows), :], ag_send.at[i], ag_rsem.at[i], (g, z, peers[i])
        )

    def norm_arrival(i):
        return remote(
            nm_own, nm.at[pl.ds(mult(sources[i] * rows, rows), rows), :], ag_send.at[i], ag_rsem.at[i], (g, z, peers[i])
        )

    for i in range(1, T):
        norm_copy(i).start()
    nm[pl.ds(mult(t * rows, rows), rows), :] = nm_own[...]
    own_upto(5 + 1 + AHEAD)
    for d in range(2, F):
        service(5, d)
    service_all(6)
    own_upto(n_chunks)
    for i in range(1, T):
        norm_arrival(i).wait_recv()

    utile = min(256, HB)

    def up_block(j):
        y_wait_all(3 + j)

        def up_step(i, carry):
            at = pl.ds(mult(i * utile, utile), utile)
            a = jnp.dot(nm[...], gu[j, :, at], preferred_element_type=jnp.float32)
            a = jnp.maximum(a, 0.0)
            hidden[:, pl.ds(mult(j * HB + i * utile, utile), utile)] = (a * a).astype(jnp.bfloat16)
            return carry

        lax.fori_loop(0, HB // utile, up_step, 0)

    for j in range(PIECES):
        if j < PIECES - 1:
            up_block(j)
        if F > 1:
            service(first_down + j, 1)
    up_block(PIECES - 1)

    ntile = min(256, N)

    def fin_copy(src, i):
        return remote(
            fin.at[src, pl.ds(mult(peers[i] * rows, rows), rows), :], rs2.at[src, i],
            fs_send.at[src, i], fs_rsem.at[src, i], (g, z, peers[i]),
        )

    def down(src):
        def down_step(i, carry):
            at = pl.ds(mult(i * ntile, ntile), ntile)
            fin[src, :, at] = jnp.dot(
                hidden[...], gd[src, :, at], preferred_element_type=jnp.float32
            ).astype(jnp.bfloat16)
            return carry

        lax.fori_loop(0, N // ntile, down_step, 0)
        for i in range(1, T):
            fin_copy(src, i).start()

    def finish(src):
        for i in range(1, T):
            fin_copy(src, i).wait_recv()
        cols = pl.ds(mult(src * N, N), N)
        total = fin[src, pl.ds(mult(t * rows, rows), rows), :].astype(jnp.float32)
        for k in range(1, T):
            total = total + rs2[src, k].astype(jnp.float32)
        out[:, cols] = (resid[:, cols] + total).astype(jnp.bfloat16)

    down(z)
    for d in range(1, F):
        if d + 1 < F:
            service(first_down, d + 1)
        for c in range(first_down, n_chunks):
            y_wait(c, d)
        both(d, lambda src, left: down(src))
        if d + 1 < F:
            for c in range(first_down + 1, n_chunks):
                service(c, d + 1)
        if d == 1:
            finish(z)
        else:
            both(d - 1, lambda src, left: finish(src))
    both(F - 1, lambda src, left: finish(src))

    for c in range(n_chunks):
        @pl.when(z < F - 1)
        def _():
            own_right(c).wait_send()

        @pl.when(z > 0)
        def _():
            own_left(c).wait_send()

        for d in range(1, F):
            def drain(src, left):
                if d < F - 1:
                    if left:
                        @pl.when(z > 0)
                        def _():
                            left_hop(c, d, src).wait_send()
                    else:
                        @pl.when(z < F - 1)
                        def _():
                            right_hop(c, d, src).wait_send()
                across(c, d, src, left).wait_send()

            both(d, drain)
    for i in range(1, T):
        stat_copy(i).wait_send()
        mix_copy(i).wait_send()
        norm_copy(i).wait_send()
        for src in range(F):
            fin_copy(src, i).wait_send()


def solution(mesh):
    F, T = mesh.shape["fs"], mesh.shape["tp"]

    def step(tokens, norm_in, w_value, w_gate, conv_kernel, ln_gain, ln_shift, w_out, norm_mlp, w_up, w_down):
        S, D = tokens.shape
        R, C = w_value.shape
        H = w_up.shape[1]
        N = w_out.shape[1]
        rows = S // T
        chunks = 3 + 2 * PIECES
        bf16, f32 = jnp.bfloat16, jnp.float32
        dma = pltpu.SemaphoreType.DMA
        vmem = pl.BlockSpec(memory_space=pltpu.VMEM)
        anywhere = pl.BlockSpec(memory_space=pl.ANY)
        return pl.pallas_call(
            functools.partial(kernel, F, T),
            out_shape=jax.ShapeDtypeStruct((rows, D), bf16),
            in_specs=[vmem] * 6 + [anywhere] * 5,
            out_specs=vmem,
            scratch_shapes=[
                pltpu.VMEM((S, D), bf16),
                pltpu.VMEM((D, C), bf16),
                pltpu.VMEM((D, C), bf16),
                pltpu.VMEM((F, C, N), bf16),
                pltpu.VMEM((PIECES, D, H // PIECES), bf16),
                pltpu.VMEM((F, H, N), bf16),
                pltpu.VMEM((S + PAD, C), f32),
                pltpu.VMEM((S, C), f32),
                pltpu.VMEM((S, C), bf16),
                pltpu.VMEM((S, D), bf16),
                pltpu.VMEM((T, rows, D), bf16),
                pltpu.VMEM((rows, D), f32),
                pltpu.VMEM((S, D), bf16),
                pltpu.VMEM((S, H), bf16),
                pltpu.VMEM((F, S, N), bf16),
                pltpu.VMEM((F, T, rows, N), bf16),
                pltpu.VMEM((8, S), f32),
                pltpu.VMEM((T, 8, S), f32),
                pltpu.VMEM((rows, D), bf16),
                dma((4 + PIECES,)),
            ]
            + [dma((chunks, F))] * 8
            + [dma((T,))] * 6
            + [dma((F, T))] * 2,
            compiler_params=pltpu.CompilerParams(
                collective_id=0, has_side_effects=True, vmem_limit_bytes=62 * 1024 * 1024
            ),
        )(
            tokens, norm_in.reshape(1, D), conv_kernel, ln_gain.reshape(1, D), ln_shift.reshape(1, D),
            norm_mlp.reshape(1, D), w_value, w_gate, w_out, w_up, w_down,
        )

    in_specs = (
        P(("grp", "fs"), None), P(), P("fs", "tp"), P("fs", "tp"), P(), P(), P(),
        P("tp", "fs"), P(), P("fs", "tp"), P("tp", "fs"),
    )
    return jax.shard_map(
        step, mesh=mesh, in_specs=in_specs, out_specs=P(("grp", "fs", "tp"), None), check_vma=False
    )
```

```python
import functools

import jax
import jax.numpy as jnp
from jax import lax
from jax.experimental import pallas as pl
from jax.experimental.pallas import tpu as pltpu
from jax.sharding import PartitionSpec as P

MESH = pl.DeviceIdType.MESH
PIECES = 4
AHEAD = 3
PAD = 32


def rms_rows(x, gain):
    return x * lax.rsqrt(jnp.mean(x * x, axis=-1, keepdims=True) + 1e-06) * gain


def kernel(
    F, T,
    tok, norm_in, conv_k, ln_gain, ln_shift, norm_mlp, wv, wg, wo, wu, wd,
    out,
    normed, gv, gg, go, gu, gd, gated, conv, act, part, rs, resid, nm, hidden, fin, rs2,
    nm_e, hid_e, fin_e, rs_e, sum_e, ret,
    st_own, st_recv, nm_own,
    local_sem, zsend_r, zsend_l, zrecv_r, zrecv_l, ysend_r, ysend_l, yrecv_r, yrecv_l,
    st_send, st_rsem, rs_send, rs_rsem, ag_send, ag_rsem, fs_send, fs_rsem,
    rest, ex_sem, ea_send, ea_rsem, fe_send, fe_rsem, ret_send, ret_rsem,
):
    g = lax.axis_index("grp")
    z = lax.axis_index("fs")
    t = lax.axis_index("tp")
    S, D = tok.shape
    R, C = wv.shape
    H = wu.shape[1]
    N = wo.shape[1]
    taps = conv_k.shape[0]
    rows = S // T
    R2, C2, H2 = R // 2, C // 2, H // 2
    HB, HC = H // PIECES, H2 // PIECES
    other = 1 - g
    n_chunks = 3 + 2 * PIECES
    first_down = 3 + PIECES

    LOW = PIECES // 2
    HL = LOW * HB
    at_left, at_right = z == 0, z == F - 1
    is_end = jnp.logical_or(at_left, at_right)
    help_left, help_right = z == 1, z == F - 2

    def upper(c):
        return c >= 3 and (c - 3) % PIECES >= LOW

    def when_right(c):
        return pl.when(z < F - 1 - upper(c))

    def when_left(c):
        return pl.when(z > 0 + upper(c))

    def for_ends(body):
        @pl.when(at_left)
        def _():
            body(z + 1)

        @pl.when(at_right)
        def _():
            body(z - 1)

    def for_helpers(body):
        @pl.when(help_left)
        def _():
            body(z - 1)

        @pl.when(help_right)
        def _():
            body(z + 1)

    def mult(i, k):
        return pl.multiple_of(i, k)

    def own(c, h):
        if c < 3:
            ref, size = ((wv, R2), (wg, R2), (wo, C2))[c]
            return ref.at[pl.ds(mult(h * size, size), size), :]
        if c < first_down:
            return wu.at[pl.ds(mult(h * R2, R2), R2), pl.ds((c - 3) * HB, HB)]
        return wd.at[pl.ds(mult((c - first_down) * HB + h * HC, HC), HC), :]

    def slot(c, src, h):
        if c < 2:
            return (gv, gg)[c].at[pl.ds(mult(src * R + h * R2, R2), R2), :]
        if c == 2:
            return go.at[src, pl.ds(mult(h * C2, C2), C2), :]
        if c < first_down:
            return gu.at[c - 3, pl.ds(mult(src * R + h * R2, R2), R2), :]
        return gd.at[src, pl.ds(mult((c - first_down) * HB + h * HC, HC), HC), :]

    def remote(src_ref, dst_ref, send, recv, device):
        return pltpu.make_async_remote_copy(
            src_ref=src_ref, dst_ref=dst_ref, send_sem=send, recv_sem=recv,
            device_id=device, device_id_type=MESH,
        )

    peers = [lax.rem(t + i, T) for i in range(T)]
    sources = [lax.rem(t - i + T, T) for i in range(T)]

    barrier = pltpu.get_barrier_semaphore()

    def greet(device):
        pl.semaphore_signal(barrier, inc=1, device_id=device, device_id_type=MESH)

    greet((other, z, t))
    for i in range(1, T):
        greet((g, z, peers[i]))

    @pl.when(z > 0)
    def _():
        greet((g, z - 1, t))

    @pl.when(z < F - 1)
    def _():
        greet((g, z + 1, t))

    ends = lax.div(z + F - 1, F) + lax.div(2 * F - 2 - z, F)
    pl.semaphore_wait(barrier, T + ends)

    ys, yr = (ysend_r, ysend_l), (yrecv_r, yrecv_l)

    def own_right(c):
        return remote(own(c, g), slot(c, z, g), zsend_r.at[c, 0], zrecv_r.at[c, 1], (g, z + 1, t))

    def own_left(c):
        return remote(own(c, g), slot(c, z, g), zsend_l.at[c, 0], zrecv_l.at[c, 1], (g, z - 1, t))

    def right_hop(c, d, src):
        return remote(slot(c, src, g), slot(c, src, g), zsend_r.at[c, d], zrecv_r.at[c, min(d + 1, F - 1)], (g, z + 1, t))

    def left_hop(c, d, src):
        return remote(slot(c, src, g), slot(c, src, g), zsend_l.at[c, d], zrecv_l.at[c, min(d + 1, F - 1)], (g, z - 1, t))

    def arrival(c, d, src, left):
        sems = zrecv_l if left else zrecv_r
        return remote(slot(c, src, g), slot(c, src, g), zsend_r.at[c, d], sems.at[c, d], (g, z, t))

    def across(c, d, src, left):
        return remote(slot(c, src, g), slot(c, src, g), ys[left].at[c, d], yr[left].at[c, d], (other, z, t))

    def across_arrival(c, d, src, left):
        return remote(slot(c, src, other), slot(c, src, other), ys[left].at[c, d], yr[left].at[c, d], (other, z, t))

    def own_rest(c, helper):
        return remote(own(c, other), slot(c, z, other), ex_sem.at[2 + c], rest.at[c], (g, helper, t))

    issued = [0]

    def own_upto(limit):
        while issued[0] < min(limit, n_chunks):
            c = issued[0]
            issued[0] += 1

            @when_right(c)
            def _():
                own_right(c).start()

            @when_left(c)
            def _():
                own_left(c).start()

            for_ends(lambda helper: own_rest(c, helper).start())

    def both(d, body, c=0):
        @pl.when(jnp.logical_and(z - d >= 0, z < F - upper(c)))
        def _():
            body(z - d, 0)

        @pl.when(jnp.logical_and(z + d < F, z >= 0 + upper(c)))
        def _():
            body(z + d, 1)

    def when_across(d, left):
        if d > 1:
            return lambda body: body()
        return pl.when(z != (F - 2 if left else 1))

    def forward(c, d, src, left, act_on):
        if d < F - 1:
            if left:
                @when_left(c)
                def _():
                    act_on(left_hop(c, d, src))
            else:
                @when_right(c)
                def _():
                    act_on(right_hop(c, d, src))

        @when_across(d, left)
        def _():
            act_on(across(c, d, src, left))

    def service(c, d):
        def body(src, left):
            arrival(c, d, src, left).wait_recv()
            forward(c, d, src, left, lambda copy: copy.start())

        both(d, body, c)

    def service_all(c):
        own_upto(c + 1 + AHEAD)
        for d in range(1, F):
            service(c, d)

    def y_wait(c, d):
        def body(src, left):
            @when_across(d, left)
            def _():
                across_arrival(c, d, src, left).wait_recv()

            if d == 1:
                @pl.when(z == (F - 2 if left else 1))
                def _():
                    remote(slot(c, src, other), slot(c, src, other), ex_sem.at[0], rest.at[c], (g, src, t)).wait_recv()

        both(d, body, c)

    def y_wait_all(c):
        for d in range(1, F):
            y_wait(c, d)

    own_upto(1)
    copies = [
        pltpu.make_async_copy(wv, gv.at[pl.ds(mult(z * R, R), R), :], local_sem.at[0]),
        pltpu.make_async_copy(wg, gg.at[pl.ds(mult(z * R, R), R), :], local_sem.at[1]),
        pltpu.make_async_copy(wo, go.at[z], local_sem.at[2]),
        pltpu.make_async_copy(wd, gd.at[z], local_sem.at[3]),
    ]
    for j in range(PIECES):
        copies.append(
            pltpu.make_async_copy(
                wu.at[:, pl.ds(j * HB, HB)], gu.at[j, pl.ds(mult(z * R, R), R), :], local_sem.at[4 + j]
            )
        )
    for copy in copies:
        copy.start()
    own_upto(1 + AHEAD)

    block = 64

    def norm_step(i, carry):
        at = pl.ds(mult(i * block, block), block)
        x = tok[at, :].astype(jnp.float32)
        normed[at, :] = rms_rows(x, norm_in[...].astype(jnp.float32)).astype(jnp.bfloat16)
        return carry

    lax.fori_loop(0, S // block, norm_step, 0)
    for copy in copies:
        copy.wait()

    service_all(0)
    service_all(1)
    own_upto(3 + AHEAD)
    service(2, 1)
    y_wait_all(0)
    y_wait_all(1)

    tile = min(256, C)
    gated[0:PAD, :] = jnp.zeros((PAD, C), jnp.float32)

    def gate_step(i, carry):
        at = pl.ds(mult(i * tile, tile), tile)
        v = jnp.dot(normed[...], gv[:, at], preferred_element_type=jnp.float32)
        a = jnp.dot(normed[...], gg[:, at], preferred_element_type=jnp.float32)
        gated[PAD:, at] = v * jax.nn.sigmoid(a)
        return carry

    lax.fori_loop(0, C // tile, gate_step, 0)

    for d in range(2, F):
        service(2, d)

    span = 128
    lead = PAD - (taps - 1)

    def conv_step(i, carry):
        base = mult(i * span, span)
        first = jnp.zeros((span, 128), jnp.float32)
        second = jnp.zeros((span, 128), jnp.float32)
        for j in range(C // 128):
            lanes = pl.ds(j * 128, 128)
            window = gated[pl.ds(base, span + PAD), lanes]
            weights = conv_k[:, pl.ds(mult(t * C + j * 128, 128), 128)]
            acc = jnp.zeros((span, 128), jnp.float32)
            for k in range(taps):
                acc = acc + weights[k : k + 1, :] * window[lead + k : lead + k + span, :]
            conv[pl.ds(base, span), lanes] = acc
            first = first + acc
            second = second + acc * acc
        lane = lax.broadcasted_iota(jnp.int32, (span, 128), 1)
        both_sums = jnp.where(
            lane == 0,
            jnp.sum(first, axis=1, keepdims=True),
            jnp.where(lane == 1, jnp.sum(second, axis=1, keepdims=True), 0.0),
        )
        st_own[:, pl.ds(base, span)] = jnp.transpose(both_sums)[0:8, :]
        return carry

    lax.fori_loop(0, S // span, conv_step, 0)

    def stat_copy(i):
        return remote(st_own, st_recv.at[i], st_send.at[i], st_rsem.at[i], (g, z, peers[i]))

    for i in range(1, T):
        stat_copy(i).start()
    service_all(3)
    for i in range(1, T):
        stat_copy(i).wait_recv()

    gain = ln_gain[:, pl.ds(mult(t * C, C), C)].astype(jnp.float32)
    shift = ln_shift[:, pl.ds(mult(t * C, C), C)].astype(jnp.float32)

    def act_step(i, carry):
        base = mult(i * span, span)
        at = pl.ds(base, span)
        sums = st_own[:, at]
        for k in range(1, T):
            sums = sums + st_recv[k, :, at]
        mean = sums[0:1, :] / D
        var = sums[1:2, :] / D - mean * mean
        scale = lax.rsqrt(var + 1e-05)
        mean_c = jnp.transpose(jnp.broadcast_to(mean, (128, span)))[:, 0:1]
        scale_c = jnp.transpose(jnp.broadcast_to(scale, (128, span)))[:, 0:1]
        n = (conv[at, :] - mean_c) * scale_c * gain + shift
        act[at, :] = (n * jax.nn.sigmoid(n)).astype(jnp.bfloat16)
        return carry

    lax.fori_loop(0, S // span, act_step, 0)
    y_wait_all(2)

    def out_step(i, carry):
        part[:, pl.ds(mult(i * N, N), N)] = jnp.dot(
            act[...], go[i], preferred_element_type=jnp.float32
        ).astype(jnp.bfloat16)
        return carry

    lax.fori_loop(0, F, out_step, 0)

    def mix_copy(i):
        return remote(
            part.at[pl.ds(mult(peers[i] * rows, rows), rows), :], rs.at[i], rs_send.at[i], rs_rsem.at[i], (g, z, peers[i])
        )

    for i in range(1, T):
        mix_copy(i).start()
    service_all(4)
    service(5, 1)
    for i in range(1, T):
        mix_copy(i).wait_recv()

    small = 32

    def resid_step(i, carry):
        at = pl.ds(mult(i * small, small), small)
        mine = pl.ds(mult(t * rows + i * small, small), small)
        total = part[mine, :].astype(jnp.float32)
        for k in range(1, T):
            total = total + rs[k, at, :].astype(jnp.float32)
        r = tok[mine, :].astype(jnp.float32) + total
        resid[at, :] = r
        nm_own[at, :] = rms_rows(r, norm_mlp[...].astype(jnp.float32)).astype(jnp.bfloat16)
        return carry

    lax.fori_loop(0, rows // small, resid_step, 0)

    def norm_copy(i):
        return remote(
            nm_own, nm.at[pl.ds(mult(t * rows, rows), rows), :], ag_send.at[i], ag_rsem.at[i], (g, z, peers[i])
        )

    def norm_arrival(i):
        return remote(
            nm_own, nm.at[pl.ds(mult(sources[i] * rows, rows), rows), :], ag_send.at[i], ag_rsem.at[i], (g, z, peers[i])
        )

    for i in range(1, T):
        norm_copy(i).start()
    mine = pl.ds(mult(t * rows, rows), rows)

    def give_copy(helper):
        return remote(nm_own, nm_e.at[mine, :], ex_sem.at[0], ex_sem.at[1], (g, helper, t))

    for_ends(lambda helper: give_copy(helper).start())
    nm[mine, :] = nm_own[...]
    own_upto(5 + 1 + AHEAD)
    for d in range(2, F):
        service(5, d)
    service_all(6)
    own_upto(n_chunks)

    def share_copy(i):
        return remote(nm_e.at[mine, :], nm_e.at[mine, :], ea_send.at[i], ea_rsem.at[i], (g, z, peers[i]))

    def share_arrival(i):
        there = pl.ds(mult(sources[i] * rows, rows), rows)
        return remote(nm_e.at[there, :], nm_e.at[there, :], ea_send.at[i], ea_rsem.at[i], (g, z, peers[i]))

    def share(end):
        remote(nm_own, nm_e.at[mine, :], ex_sem.at[0], ex_sem.at[1], (g, end, t)).wait_recv()
        for i in range(1, T):
            share_copy(i).start()

    for_helpers(share)
    for i in range(1, T):
        norm_arrival(i).wait_recv()

    utile = min(256, HB)

    def up_block(j):
        y_wait_all(3 + j)

        def up_step(i, carry):
            at = pl.ds(mult(i * utile, utile), utile)
            a = jnp.dot(nm[...], gu[j, :, at], preferred_element_type=jnp.float32)
            a = jnp.maximum(a, 0.0)
            hidden[:, pl.ds(mult(j * HB + i * utile, utile), utile)] = (a * a).astype(jnp.bfloat16)
            return carry

        lax.fori_loop(0, HB // utile, up_step, 0)

    def up_some(j):
        if j < LOW:
            up_block(j)
        else:
            @pl.when(jnp.logical_not(is_end))
            def _():
                up_block(j)

    for j in range(PIECES):
        if j < PIECES - 1:
            up_some(j)
        service(first_down + j, 1)
    up_some(PIECES - 1)

    def up_for_end(end):
        for i in range(1, T):
            share_arrival(i).wait_recv()
        per = HB // utile

        def up_step(i, carry):
            at = pl.ds(mult(lax.rem(i, per) * utile, utile), utile)
            a = jnp.dot(nm_e[...], gu[LOW + lax.div(i, per), :, at], preferred_element_type=jnp.float32)
            a = jnp.maximum(a, 0.0)
            hid_e[:, pl.ds(mult(i * utile, utile), utile)] = (a * a).astype(jnp.bfloat16)
            return carry

        lax.fori_loop(0, (PIECES - LOW) * per, up_step, 0)

    for_helpers(up_for_end)

    ntile = min(256, N)

    def fin_copy(src, i):
        return remote(
            fin.at[src, pl.ds(mult(peers[i] * rows, rows), rows), :], rs2.at[src, i],
            fs_send.at[src, i], fs_rsem.at[src, i], (g, z, peers[i]),
        )

    def end_copy(src, i):
        return remote(
            fin_e.at[src, pl.ds(mult(peers[i] * rows, rows), rows), :], rs_e.at[src, i],
            fe_send.at[src, i], fe_rsem.at[src, i], (g, z, peers[i]),
        )

    def down_for_end(src):
        def down_step(i, carry):
            at = pl.ds(mult(i * ntile, ntile), ntile)
            fin_e[src, :, at] = jnp.dot(
                hid_e[...], gd[src, HL:, at], preferred_element_type=jnp.float32
            ).astype(jnp.bfloat16)
            return carry

        lax.fori_loop(0, N // ntile, down_step, 0)
        for i in range(1, T):
            end_copy(src, i).start()

    def ret_copy(src, end):
        return remote(sum_e.at[src], ret.at[src], ret_send.at[src], ret_rsem.at[src], (g, end, t))

    def return_sum(src):
        def body(end):
            for i in range(1, T):
                end_copy(src, i).wait_recv()
            total = fin_e[src, mine, :].astype(jnp.float32)
            for k in range(1, T):
                total = total + rs_e[src, k].astype(jnp.float32)
            sum_e[src] = total.astype(jnp.bfloat16)
            ret_copy(src, end).start()

        for_helpers(body)

    def down(src):
        for_helpers(lambda end: down_for_end(src))

        def rows_to(limit):
            def down_step(i, carry):
                at = pl.ds(mult(i * ntile, ntile), ntile)
                fin[src, :, at] = jnp.dot(
                    hidden[:, :limit], gd[src, :limit, at], preferred_element_type=jnp.float32
                ).astype(jnp.bfloat16)
                return carry

            lax.fori_loop(0, N // ntile, down_step, 0)

        @pl.when(is_end)
        def _():
            rows_to(HL)

        @pl.when(jnp.logical_not(is_end))
        def _():
            rows_to(H)

        for i in range(1, T):
            fin_copy(src, i).start()

    def finish(src):
        for i in range(1, T):
            fin_copy(src, i).wait_recv()
        cols = pl.ds(mult(src * N, N), N)
        total = fin[src, mine, :].astype(jnp.float32)
        for k in range(1, T):
            total = total + rs2[src, k].astype(jnp.float32)
        resid[:, cols] = resid[:, cols] + total

    down(z)
    for d in range(1, F):
        if d + 1 < F:
            service(first_down, d + 1)
        for c in range(first_down, n_chunks):
            y_wait(c, d)
        both(d, lambda src, left: down(src))
        if d + 1 < F:
            for c in range(first_down + 1, n_chunks):
                service(c, d + 1)
        if d == 1:
            return_sum(z)
        else:
            both(d - 1, lambda src, left: return_sum(src))
    both(F - 1, lambda src, left: return_sum(src))

    def finish_step(src, carry):
        finish(src)

        def add(helper):
            cols = pl.ds(mult(src * N, N), N)
            ret_copy(src, helper).wait_recv()
            resid[:, cols] = resid[:, cols] + ret[src].astype(jnp.float32)

        for_ends(add)
        cols = pl.ds(mult(src * N, N), N)
        out[:, cols] = resid[:, cols].astype(jnp.bfloat16)
        return carry

    lax.fori_loop(0, F, finish_step, 0)

    for c in range(n_chunks):
        @when_right(c)
        def _():
            own_right(c).wait_send()

        @when_left(c)
        def _():
            own_left(c).wait_send()

        for_ends(lambda helper: own_rest(c, helper).wait_send())

        for d in range(1, F):
            both(d, lambda src, left: forward(c, d, src, left, lambda copy: copy.wait_send()), c)

    for_ends(lambda helper: give_copy(helper).wait_send())

    def drain_helper(end):
        for i in range(1, T):
            share_copy(i).wait_send()
            for src in range(F):
                end_copy(src, i).wait_send()
        for src in range(F):
            ret_copy(src, end).wait_send()

    for_helpers(drain_helper)
    for i in range(1, T):
        stat_copy(i).wait_send()
        mix_copy(i).wait_send()
        norm_copy(i).wait_send()
        for src in range(F):
            fin_copy(src, i).wait_send()


def solution(mesh):
    F, T = mesh.shape["fs"], mesh.shape["tp"]

    def step(tokens, norm_in, w_value, w_gate, conv_kernel, ln_gain, ln_shift, w_out, norm_mlp, w_up, w_down):
        S, D = tokens.shape
        R, C = w_value.shape
        H = w_up.shape[1]
        N = w_out.shape[1]
        rows = S // T
        chunks = 3 + 2 * PIECES
        bf16, f32 = jnp.bfloat16, jnp.float32
        dma = pltpu.SemaphoreType.DMA
        vmem = pl.BlockSpec(memory_space=pltpu.VMEM)
        anywhere = pl.BlockSpec(memory_space=pl.ANY)
        return pl.pallas_call(
            functools.partial(kernel, F, T),
            out_shape=jax.ShapeDtypeStruct((rows, D), bf16),
            in_specs=[vmem] * 6 + [anywhere] * 5,
            out_specs=vmem,
            scratch_shapes=[
                pltpu.VMEM((S, D), bf16),
                pltpu.VMEM((D, C), bf16),
                pltpu.VMEM((D, C), bf16),
                pltpu.VMEM((F, C, N), bf16),
                pltpu.VMEM((PIECES, D, H // PIECES), bf16),
                pltpu.VMEM((F, H, N), bf16),
                pltpu.VMEM((S + PAD, C), f32),
                pltpu.VMEM((S, C), f32),
                pltpu.VMEM((S, C), bf16),
                pltpu.VMEM((S, D), bf16),
                pltpu.VMEM((T, rows, D), bf16),
                pltpu.VMEM((rows, D), f32),
                pltpu.VMEM((S, D), bf16),
                pltpu.VMEM((S, H), bf16),
                pltpu.VMEM((F, S, N), bf16),
                pltpu.VMEM((F, T, rows, N), bf16),
                pltpu.VMEM((S, D), bf16),
                pltpu.VMEM((S, H - H // PIECES * (PIECES // 2)), bf16),
                pltpu.VMEM((F, S, N), bf16),
                pltpu.VMEM((F, T, rows, N), bf16),
                pltpu.VMEM((F, rows, N), bf16),
                pltpu.VMEM((F, rows, N), bf16),
                pltpu.VMEM((8, S), f32),
                pltpu.VMEM((T, 8, S), f32),
                pltpu.VMEM((rows, D), bf16),
                dma((4 + PIECES,)),
            ]
            + [dma((chunks, F))] * 8
            + [dma((T,))] * 6
            + [dma((F, T))] * 2
            + [dma((chunks,)), dma((2 + chunks,)), dma((T,)), dma((T,))]
            + [dma((F, T))] * 2
            + [dma((F,))] * 2,
            compiler_params=pltpu.CompilerParams(
                collective_id=0, has_side_effects=True, vmem_limit_bytes=62 * 1024 * 1024
            ),
        )(
            tokens, norm_in.reshape(1, D), conv_kernel, ln_gain.reshape(1, D), ln_shift.reshape(1, D),
            norm_mlp.reshape(1, D), w_value, w_gate, w_out, w_up, w_down,
        )

    in_specs = (
        P(("grp", "fs"), None), P(), P("fs", "tp"), P("fs", "tp"), P(), P(), P(),
        P("tp", "fs"), P(), P("fs", "tp"), P("tp", "fs"),
    )
    return jax.shard_map(
        step, mesh=mesh, in_specs=in_specs, out_specs=P(("grp", "fs", "tp"), None), check_vma=False
    )
```
